32 devices in a mesh: rep: 2 (over x), fs: 4 (over z), tp: 4 (over y, core).
Axes of the slice: x: 2, y: 2, z: 4, core: 2. Of those that a mesh axis runs over, the one named last changes fastest.
Arguments:
- tokens: bfloat16 [8192, 2048], P(('rep', 'fs', 'tp')), may hold values from -6 to 6
- cotangent: bfloat16 [8192, 2048], P(('rep', 'fs', 'tp')), may hold values from -6 to 6
- gate_weight: bfloat16 [2048, 3072], P('fs', 'tp'), may hold values from -0.125 to 0.125
- up_weight: bfloat16 [2048, 3072], P('fs', 'tp'), may hold values from -0.125 to 0.125
- down_weight: bfloat16 [3072, 2048], P('tp', 'fs'), may hold values from -0.109375 to 0.109375
Outputs:
- grad_tokens: bfloat16 [8192, 2048], P(('rep', 'fs', 'tp'))
- grad_gate: float32 [2048, 3072], P('fs', 'tp')
- grad_up: float32 [2048, 3072], P('fs', 'tp')
- grad_down: float32 [3072, 2048], P('tp', 'fs')
- gate_row_norms: float32 [2048], P('fs')
- up_row_norms: float32 [2048], P('fs')
- down_row_norms: float32 [3072], P('tp')
The draws below stay inside these ranges and needn't reach their ends.
All inputs are finite; a program needn't handle non-finite values.
Results may differ from the reference program's by a relative error of at most 0.014.
Values may be sent and summed in bfloat16 or wider, within the bound.
A program may use at most 128 MiB of HBM per device.

```python
import jax
import jax.numpy as jnp
from jax import lax

D = 2048
FF = 3072
TOKENS = 8192
N_TP = 4


def strengthened(entries, stream_key, source, target, blocks, factor):
    owner, partner = [(jnp.arange(entries.shape[dim]) // (entries.shape[dim] // blocks)).reshape([-1 if axis == dim else 1 for axis in range(entries.ndim)]) for dim in (source, target)]
    chosen = jax.random.permutation(stream_key, blocks)[partner]
    strong = (owner == chosen) | (owner == (partner + blocks // 2) % blocks)
    return jnp.where(strong, factor * entries, entries)


def shard_levels(rng, dims, pieces, low, largest):
    factor_of, own = 1.0, jax.random.fold_in(rng, 6)
    for dim, parts in pieces:
        draws = jnp.exp(jax.random.uniform(jax.random.fold_in(own, dim), (parts,), jnp.float32, low / len(pieces), largest / len(pieces)))
        factor_of = factor_of * jnp.repeat(draws, dims[dim] // parts).reshape([-1 if axis == dim else 1 for axis in range(len(dims))])
    return factor_of


def centred(stream_key, dims, scale, reach, cuts=(), held_as=jnp.bfloat16):
    loudness = shard_levels(stream_key, dims, cuts, -0.22, 0.18) if cuts else 1.0
    drawn = jax.random.normal(stream_key, dims, jnp.float32) * scale * loudness
    return jnp.minimum(jnp.maximum(drawn, -reach), reach).astype(held_as)


def gaussian_with(key, extent, spread, most, pieces, heavy, dtype=jnp.bfloat16):
    drawn = spread * jax.random.normal(key, extent, jnp.float32)
    if pieces:
        drawn = drawn * shard_levels(key, extent, pieces, -0.22, 0.18)
    return jnp.clip(strengthened(drawn, jax.random.fold_in(key, 3), *heavy), -most, most).astype(dtype)


def setup_inputs(seed: int = 0) -> dict:
    arg_keys = jax.random.split(jax.random.key(seed), 6)
    return {
        "tokens": centred(arg_keys[0], (TOKENS, D), 1.0, 6.0, ((0, 32),)),
        "cotangent": gaussian_with(arg_keys[1], (TOKENS, D), 1.0, 6.0, ((0, 32),), (0, 1, 32, 2.75)),
        "gate_weight": centred(arg_keys[2], (D, FF), D ** -0.5, 0.125, ((0, 4), (1, 4))),
        "up_weight": centred(arg_keys[3], (D, FF), D ** -0.5, 0.125, ((0, 4), (1, 4))),
        "down_weight": centred(arg_keys[4], (FF, D), FF ** -0.5, 0.109375, ((0, 4), (1, 4))),
    }


def reference(tokens, cotangent, gate_weight, up_weight, down_weight):
    gate = jnp.dot(tokens, gate_weight, preferred_element_type=jnp.float32)
    up = jnp.dot(tokens, up_weight, preferred_element_type=jnp.float32)
    sig = jax.nn.sigmoid(gate)
    act = gate * sig
    hidden = (act * up).astype(jnp.bfloat16)
    dhid = jnp.dot(cotangent, down_weight.T, preferred_element_type=jnp.float32)
    dgate = (dhid * up * sig * (1.0 + gate * (1.0 - sig))).astype(jnp.bfloat16)
    dup = (dhid * act).astype(jnp.bfloat16)
    grad_down = jnp.dot(hidden.T, cotangent, preferred_element_type=jnp.float32)
    grad_gate = jnp.dot(tokens.T, dgate, preferred_element_type=jnp.float32)
    grad_up = jnp.dot(tokens.T, dup, preferred_element_type=jnp.float32)
    block_width = FF // N_TP
    total = jnp.zeros(tokens.shape, jnp.float32)
    for block in range(N_TP):
        lower = block * block_width
        upper = lower + block_width
        partial_term = jnp.dot(dgate[:, lower:upper], gate_weight[:, lower:upper].T, preferred_element_type=jnp.float32)
        partial_term = partial_term + jnp.dot(dup[:, lower:upper], up_weight[:, lower:upper].T, preferred_element_type=jnp.float32)
        rounded = lax.optimization_barrier(partial_term.astype(jnp.bfloat16))
        total = total + rounded.astype(jnp.float32)
    grad_tokens = total.astype(jnp.bfloat16)
    gate_row_norms = jnp.sum(grad_gate * grad_gate, axis=1)
    up_row_norms = jnp.sum(grad_up * grad_up, axis=1)
    down_row_norms = jnp.sum(grad_down * grad_down, axis=1)
    return (grad_tokens, grad_gate, grad_up, grad_down, gate_row_norms, up_row_norms, down_row_norms)
```

```python
import functools

import jax
import jax.numpy as jnp
from jax import lax
from jax.sharding import PartitionSpec as P


F32, BF16 = jnp.float32, jnp.bfloat16


def contract_last(left, right):
    return lax.dot_general(
        left, right, (((1,), (1,)), ((), ())), preferred_element_type=F32
    )


def contract_first(left, right):
    return lax.dot_general(
        left, right, (((0,), (0,)), ((), ())), preferred_element_type=F32
    )


def shift(array, axis, by):
    n = lax.axis_size(axis)
    return lax.ppermute(array, axis, [(i, (i + by) % n) for i in range(n)])


def pair(array, axis):
    n = lax.axis_size(axis)
    return lax.ppermute(array, axis, [(i, i ^ 1) for i in range(n)])


def half_of(array, index):
    size = array.shape[0] // 2
    return lax.dynamic_slice_in_dim(array, index * size, size, 0)


def gather_rows(block):
    n = lax.axis_size("tp")
    mine = [block] + [shift(block, "tp", 2 * m) for m in range(1, n // 2)]
    other = [pair(part, "tp") for part in mine]
    return jnp.concatenate(mine + other, axis=0)


def scatter_rows(partial, rows):
    n = lax.axis_size("tp")
    half = n // 2
    take = lambda i: partial[i * rows : (i + 1) * rows]
    total = None
    for m in list(range(1, half)) + [0]:
        both = take(m).astype(F32) + pair(take(half + m), "tp").astype(F32)
        if m:
            both = shift(both.astype(BF16), "tp", -2 * m).astype(F32)
        total = both if total is None else total + both
    return total.astype(BF16)


def gather_weight(shard, after=None):
    n = lax.axis_size("fs")
    f, r = lax.axis_index("fs"), lax.axis_index("rep")
    half_rows = shard.shape[0] // 2
    held = half_of(shard, r)
    if after is not None:
        held, _ = lax.optimization_barrier((held, after))
    pieces = []
    for s in range(1, n):
        held = shift(held, "fs", 1)
        pieces.append((lax.rem(f - s + n, n), held, shift(held, "rep", 1)))
    whole = jnp.zeros((n,) + shard.shape, shard.dtype)
    whole = lax.dynamic_update_slice(whole, shard[None], (f, 0, 0))
    for owner, mine, other in pieces:
        whole = lax.dynamic_update_slice(whole, mine[None], (owner, r * half_rows, 0))
        whole = lax.dynamic_update_slice(whole, other[None], (owner, (1 - r) * half_rows, 0))
    return whole, held


def rep_ordered(mine, other):
    first = lax.axis_index("rep") == 0
    return jnp.where(first, mine, other), jnp.where(first, other, mine)


def scatter_columns(part):
    n = lax.axis_size("fs")
    f = lax.axis_index("fs")
    size = part.shape[1] // n
    total = None
    for k in range(n):
        owner = lax.rem(f - 1 - k + n, n)
        block = lax.dynamic_slice_in_dim(part, owner * size, size, 1)
        if total is not None:
            block = (block.astype(F32) + shift(total, "fs", 1).astype(F32)).astype(BF16)
        total = block
    first, second = rep_ordered(total, shift(total, "rep", 1))
    return first.astype(F32) + second.astype(F32)


def sum_over(values, axis):
    n = lax.axis_size(axis)
    me = lax.axis_index(axis)
    table = jnp.zeros((n,) + values.shape, F32)
    table = lax.dynamic_update_slice(table, values[None], (me, 0))
    for s in range(1, n):
        got = shift(values, axis, s)
        table = lax.dynamic_update_slice(table, got[None], (lax.rem(me - s + n, n), 0))
    return jnp.sum(table, axis=0)


def scatter_rows_of_weight(part):
    n = lax.axis_size("fs")
    f, r = lax.axis_index("fs"), lax.axis_index("rep")
    size = part.shape[0] // n
    rows = size // 2
    total = None
    for k in range(n):
        owner = lax.rem(f - 1 - k + n, n)
        take = lambda half: lax.dynamic_slice_in_dim(part, owner * size + half * rows, rows, 0)
        both = take(r).astype(F32) + shift(take(1 - r), "rep", 1).astype(F32)
        if total is not None:
            both = both + shift(total, "fs", 1).astype(F32)
        total = both.astype(BF16)
    return jnp.concatenate(rep_ordered(total, shift(total, "rep", 1)), axis=0).astype(F32)


def local(tokens, cotangent, gate_weight, up_weight, down_weight):
    group_tokens = gather_rows(tokens)
    group_cotangent = gather_rows(cotangent)
    gate_blocks, last_gate = gather_weight(gate_weight)
    up_blocks, _ = gather_weight(up_weight)
    down_blocks, _ = gather_weight(down_weight, after=last_gate)
    whole_gate = gate_blocks.reshape((-1, gate_weight.shape[1]))
    whole_up = up_blocks.reshape((-1, up_weight.shape[1]))
    whole_down = jnp.concatenate(list(down_blocks), axis=1)
    gate = jnp.dot(group_tokens, whole_gate, preferred_element_type=F32)
    up = jnp.dot(group_tokens, whole_up, preferred_element_type=F32)
    sig = jax.nn.sigmoid(gate)
    act = gate * sig
    hidden = (act * up).astype(BF16)
    part_down = contract_first(hidden, group_cotangent).astype(BF16)
    grad_down = scatter_columns(part_down)
    dhid = contract_last(group_cotangent, whole_down)
    dgate = (dhid * up * sig * (1.0 + gate * (1.0 - sig))).astype(BF16)
    dup = (dhid * act).astype(BF16)
    part_gate = contract_first(group_tokens, dgate).astype(BF16)
    grad_gate = scatter_rows_of_weight(part_gate)
    part_up = contract_first(group_tokens, dup).astype(BF16)
    grad_up = scatter_rows_of_weight(part_up)
    partial = (contract_last(dgate, whole_gate) + contract_last(dup, whole_up)).astype(BF16)
    grad_tokens = scatter_rows(partial, tokens.shape[0])
    down_row_norms = sum_over(jnp.sum(grad_down * grad_down, axis=1), "fs")
    gate_row_norms = sum_over(jnp.sum(grad_gate * grad_gate, axis=1), "tp")
    up_row_norms = sum_over(jnp.sum(grad_up * grad_up, axis=1), "tp")
    return (
        grad_tokens,
        grad_gate,
        grad_up,
        grad_down,
        gate_row_norms,
        up_row_norms,
        down_row_norms,
    )


def solution(mesh):
    placed = (
        P(("rep", "fs", "tp"), None),
        P(("rep", "fs", "tp"), None),
        P("fs", "tp"),
        P("fs", "tp"),
        P("tp", "fs"),
    )
    return jax.shard_map(
        local,
        mesh=mesh,
        in_specs=placed,
        out_specs=(
            P(("rep", "fs", "tp"), None),
            P("fs", "tp"),
            P("fs", "tp"),
            P("tp", "fs"),
            P("fs"),
            P("fs"),
            P("tp"),
        ),
        check_vma=False,
    )
```

```python
import functools

import jax
import jax.numpy as jnp
from jax import lax
from jax.sharding import PartitionSpec as P


F32, BF16 = jnp.float32, jnp.bfloat16


def contract_last(left, right):
    return lax.dot_general(
        left, right, (((1,), (1,)), ((), ())), preferred_element_type=F32
    )


def contract_first(left, right):
    return lax.dot_general(
        left, right, (((0,), (0,)), ((), ())), preferred_element_type=F32
    )


def shift(array, axis, by):
    n = lax.axis_size(axis)
    return lax.ppermute(array, axis, [(i, (i + by) % n) for i in range(n)])


def pair(array, axis):
    n = lax.axis_size(axis)
    return lax.ppermute(array, axis, [(i, i ^ 1) for i in range(n)])


def half_of(array, index):
    size = array.shape[0] // 2
    return lax.dynamic_slice_in_dim(array, index * size, size, 0)


def gather_rows(block):
    n = lax.axis_size("tp")
    mine = [block] + [shift(block, "tp", 2 * m) for m in range(1, n // 2)]
    other = [pair(part, "tp") for part in mine]
    return jnp.concatenate(mine + other, axis=0)


def scatter_rows(partial, rows):
    n = lax.axis_size("tp")
    half = n // 2
    take = lambda i: partial[i * rows : (i + 1) * rows]
    total = None
    for m in list(range(1, half)) + [0]:
        both = take(m).astype(F32) + pair(take(half + m), "tp").astype(F32)
        if m:
            both = shift(both.astype(BF16), "tp", -2 * m).astype(F32)
        total = both if total is None else total + both
    return total.astype(BF16)


def gather_weight(shard, after=None):
    n = lax.axis_size("fs")
    f, r = lax.axis_index("fs"), lax.axis_index("rep")
    half_rows = shard.shape[0] // 2
    held = half_of(shard, r)
    if after is not None:
        held, _ = lax.optimization_barrier((held, after))
    pieces = []
    for s in range(1, n):
        held = shift(held, "fs", 1)
        pieces.append((lax.rem(f - s + n, n), held, shift(held, "rep", 1)))
    whole = jnp.zeros((n,) + shard.shape, shard.dtype)
    whole = lax.dynamic_update_slice(whole, shard[None], (f, 0, 0))
    for owner, mine, other in pieces:
        whole = lax.dynamic_update_slice(whole, mine[None], (owner, r * half_rows, 0))
        whole = lax.dynamic_update_slice(whole, other[None], (owner, (1 - r) * half_rows, 0))
    return whole, held


def rep_ordered(mine, other):
    first = lax.axis_index("rep") == 0
    return jnp.where(first, mine, other), jnp.where(first, other, mine)


def scatter_columns(part):
    n = lax.axis_size("fs")
    f = lax.axis_index("fs")
    size = part.shape[1] // n
    total = None
    sums = []
    for k in range(n):
        owner = lax.rem(f - 1 - k + n, n)
        block = lax.dynamic_slice_in_dim(part, owner * size, size, 1)
        if total is not None:
            block = (block.astype(F32) + shift(total, "fs", 1).astype(F32)).astype(BF16)
        total = block
        sums.append(total)
    first, second = rep_ordered(total, shift(total, "rep", 1))
    return first.astype(F32) + second.astype(F32), sums


def held_until(array, ready):
    return lax.optimization_barrier((array, ready))[0]


def sum_over(values, axis):
    n = lax.axis_size(axis)
    me = lax.axis_index(axis)
    table = jnp.zeros((n,) + values.shape, F32)
    table = lax.dynamic_update_slice(table, values[None], (me, 0))
    for s in range(1, n):
        got = shift(values, axis, s)
        table = lax.dynamic_update_slice(table, got[None], (lax.rem(me - s + n, n), 0))
    return jnp.sum(table, axis=0)


def scatter_rows_of_weight(part):
    n = lax.axis_size("fs")
    f, r = lax.axis_index("fs"), lax.axis_index("rep")
    size = part.shape[0] // n
    rows = size // 2
    total = None
    for k in range(n):
        owner = lax.rem(f - 1 - k + n, n)
        take = lambda half: lax.dynamic_slice_in_dim(part, owner * size + half * rows, rows, 0)
        both = take(r).astype(F32) + shift(take(1 - r), "rep", 1).astype(F32)
        if total is not None:
            both = both + shift(total, "fs", 1).astype(F32)
        total = both.astype(BF16)
    return jnp.concatenate(rep_ordered(total, shift(total, "rep", 1)), axis=0).astype(F32)


def local(tokens, cotangent, gate_weight, up_weight, down_weight):
    group_tokens = gather_rows(tokens)
    group_cotangent = gather_rows(cotangent)
    gate_blocks, last_gate = gather_weight(gate_weight)
    up_blocks, _ = gather_weight(up_weight)
    down_blocks, _ = gather_weight(down_weight, after=last_gate)
    whole_gate = gate_blocks.reshape((-1, gate_weight.shape[1]))
    whole_up = up_blocks.reshape((-1, up_weight.shape[1]))
    whole_down = jnp.concatenate(list(down_blocks), axis=1)
    gate = jnp.dot(group_tokens, whole_gate, preferred_element_type=F32)
    up = jnp.dot(group_tokens, whole_up, preferred_element_type=F32)
    sig = jax.nn.sigmoid(gate)
    act = gate * sig
    hidden = (act * up).astype(BF16)
    part_down = contract_first(hidden, group_cotangent).astype(BF16)
    grad_down, down_sums = scatter_columns(part_down)
    dhid = contract_last(group_cotangent, whole_down)
    dgate = (dhid * up * sig * (1.0 + gate * (1.0 - sig))).astype(BF16)
    dup = (dhid * act).astype(BF16)
    dgate, dup = lax.optimization_barrier((dgate, dup, down_sums[1]))[:2]
    part_gate = contract_first(group_tokens, dgate).astype(BF16)
    grad_gate = scatter_rows_of_weight(part_gate)
    partial = (contract_last(dgate, whole_gate) + contract_last(dup, whole_up)).astype(BF16)
    part_up = contract_first(group_tokens, held_until(dup, (partial, down_sums[2]))).astype(BF16)
    grad_up = scatter_rows_of_weight(part_up)
    grad_tokens = scatter_rows(partial, tokens.shape[0])
    down_row_norms = sum_over(jnp.sum(grad_down * grad_down, axis=1), "fs")
    gate_row_norms = sum_over(jnp.sum(grad_gate * grad_gate, axis=1), "tp")
    up_row_norms = sum_over(jnp.sum(grad_up * grad_up, axis=1), "tp")
    return (
        grad_tokens,
        grad_gate,
        grad_up,
        grad_down,
        gate_row_norms,
        up_row_norms,
        down_row_norms,
    )


def solution(mesh):
    placed = (
        P(("rep", "fs", "tp"), None),
        P(("rep", "fs", "tp"), None),
        P("fs", "tp"),
        P("fs", "tp"),
        P("tp", "fs"),
    )
    return jax.shard_map(
        local,
        mesh=mesh,
        in_specs=placed,
        out_specs=(
            P(("rep", "fs", "tp"), None),
            P("fs", "tp"),
            P("fs", "tp"),
            P("tp", "fs"),
            P("fs"),
            P("fs"),
            P("tp"),
        ),
        check_vma=False,
    )
```
